32 devices in a mesh: sp: 16 (over z, y, x), tp: 2 (over core).
Axes of the slice: x: 2, y: 2, z: 4, core: 2. Of those that a mesh axis runs over, the one named last changes fastest.
Arguments:
- latent: bfloat16 [4096, 2048], P(('sp', 'tp')), may hold values from -3 to 3
- context: bfloat16 [1024, 2048], P('sp'), may hold values from -6 to 6
- condition: float32 [2048], replicated, may hold values from -6 to 6
- ctx_cond: float32 [2048], replicated, may hold values from -6 to 6
- norm_gain: float32 [2048], replicated, may hold values from 0.1 to 1.9
- w_shift: bfloat16 [2048, 2048], P('sp', 'tp'), may hold values from -0.25 to 0.25
- w_scale: bfloat16 [2048, 2048], P('sp', 'tp'), may hold values from -0.25 to 0.25
- w_gate: bfloat16 [2048, 2048], P('sp', 'tp'), may hold values from -0.25 to 0.25
- w_query: bfloat16 [2048, 2048], P(None, 'tp'), may hold values from -0.125 to 0.125
- w_key: bfloat16 [2048, 2048], P(None, 'tp'), may hold values from -0.125 to 0.125
- w_value: bfloat16 [2048, 2048], P(None, 'tp'), may hold values from -0.125 to 0.125
- w_out: bfloat16 [2048, 2048], P('tp'), may hold values from -0.125 to 0.125
- rel_bias: float32 [16, 15, 31], replicated, may hold values from 2 to 250
Outputs:
- updated: bfloat16 [4096, 2048], P(('sp', 'tp'))
The draws below stay inside these ranges and needn't reach their ends.
All inputs are finite; a program needn't handle non-finite values.
Results may differ from the reference program's by a relative error of at most 0.015.
Values may be sent and summed in bfloat16 or wider, within the bound.
A program may use at most 128 MiB of HBM per device.

```python
import jax
import jax.numpy as jnp
import numpy as np
from jax import lax

D = 2048
HEADS = 16
HEAD_DIM = 128
GRID_W = 32
WIN_H = 8
WIN_W = 16
CTX = 1024
TOKENS = 4096
N_TP = 2


def draw_rel_bias(key, part):
    drawn = jax.random.uniform(key, (HEADS, 2 * WIN_H - 1, 2 * WIN_W - 1), jnp.float32, 2.0, 4.0)
    return drawn


def steps_of(stream_key, dims, split, low, largest):
    loudness, own = 1.0, jax.random.fold_in(stream_key, 6)
    for axis_at, blocks in split:
        steps = jnp.exp(jax.random.uniform(jax.random.fold_in(own, axis_at), (blocks,), jnp.float32, low / len(split), largest / len(split)))
        loudness = loudness * jnp.repeat(steps, dims[axis_at] // blocks).reshape([-1 if axis == axis_at else 1 for axis in range(len(dims))])
    return loudness


def noise(own_key, dims, deviation, limit, shards=(), held_as=jnp.bfloat16):
    level = steps_of(own_key, dims, shards, -0.22, 0.18) if shards else 1.0
    values = jax.random.normal(own_key, dims, jnp.float32) * deviation * level
    return jnp.minimum(jnp.maximum(values, -limit), limit).astype(held_as)


def setup_inputs(seed: int = 0) -> dict:
    splits = jax.random.split(jax.random.key(seed), 14)
    return {
        "latent": noise(splits[0], (TOKENS, D), 0.5, 3.0, ((0, 32),)),
        "context": noise(splits[1], (CTX, D), 1.0, 6.0, ((0, 16),)),
        "condition": noise(splits[2], (D,), 1.0, 6.0, (), jnp.float32),
        "ctx_cond": noise(splits[3], (D,), 1.0, 6.0, (), jnp.float32),
        "norm_gain": jnp.clip(1.0 + 0.18 * jax.random.normal(splits[4], (D,), jnp.float32), 0.1, 1.9),
        "w_shift": noise(splits[5], (D, D), (D // 4) ** -0.5, 0.25, ((0, 16), (1, 2))),
        "w_scale": noise(splits[6], (D, D), (D // 4) ** -0.5, 0.25, ((0, 16), (1, 2))),
        "w_gate": noise(splits[7], (D, D), (D // 4) ** -0.5, 0.25, ((0, 16), (1, 2))),
        "w_query": noise(splits[8], (D, D), D ** -0.5, 0.125, ((1, 2),)),
        "w_key": noise(splits[9], (D, D), D ** -0.5, 0.125, ((1, 2),)),
        "w_value": noise(splits[10], (D, D), D ** -0.5, 0.125, ((1, 2),)),
        "w_out": noise(splits[11], (D, D), D ** -0.5, 0.125, ((0, 2),)),
        "rel_bias": draw_rel_bias(jax.random.fold_in(splits[13], 71), 0),
    }


NORM_EPS = 1e-06
NEG_BIG = -1e+30

def rms_mod(block, norm_gain, shifts, scales):
    block = block.astype(jnp.float32)
    normed = block * lax.rsqrt(lax.optimization_barrier(jnp.mean(block * block, axis=-1, keepdims=True)) + NORM_EPS) * norm_gain
    return (normed * (1.0 + scales) + shifts).astype(jnp.bfloat16)

def project(block, weight):
    return jnp.dot(block, weight, preferred_element_type=jnp.float32).astype(jnp.bfloat16)

def geometry(total_rows):
    row_ids = np.arange(total_rows)
    starts = np.clip(row_ids - WIN_H // 2, 0, total_rows - WIN_H)
    row_index = starts[:, None] + np.arange(WIN_H)[None, :]
    row_off = row_index - row_ids[:, None] + WIN_H - 1
    col_ids = np.arange(GRID_W)
    col_start = np.clip(col_ids - WIN_W // 2, 0, GRID_W - WIN_W)
    col_in = (col_ids[None, :] >= col_start[:, None]) & (col_ids[None, :] < col_start[:, None] + WIN_W)
    col_off = np.clip(col_ids[None, :] - col_ids[:, None], 1 - WIN_W, WIN_W - 1) + WIN_W - 1
    return (row_index, row_off, col_in, col_off)

def reference(latent, context, condition, ctx_cond, norm_gain, w_shift, w_scale, w_gate, w_query, w_key, w_value, w_out, rel_bias):
    activated = jax.nn.silu(jnp.stack([condition, ctx_cond])).astype(jnp.bfloat16)
    shifts = jnp.dot(activated, w_shift, preferred_element_type=jnp.float32)
    scales = jnp.dot(activated, w_scale, preferred_element_type=jnp.float32)
    gate_vec = jnp.dot(activated[:1], w_gate, preferred_element_type=jnp.float32)[0]
    normed = rms_mod(latent, norm_gain, shifts[0], scales[0])
    ctx_normed = rms_mod(context, norm_gain, shifts[1], scales[1])
    queries = project(normed, w_query)
    lat_keys = project(normed, w_key)
    lat_values = project(normed, w_value)
    ctx_keys = project(ctx_normed, w_key)
    ctx_values = project(ctx_normed, w_value)
    total_rows = latent.shape[0] // GRID_W
    row_index, row_off, col_in, col_off = geometry(total_rows)
    inv_scale = HEAD_DIM ** (-0.5)

    def grid_heads(array):
        return jnp.transpose(array.reshape(total_rows, GRID_W, HEADS, HEAD_DIM), (2, 0, 1, 3))

    def ctx_heads(array):
        return jnp.transpose(array.reshape(-1, HEADS, HEAD_DIM), (1, 0, 2))

    def per_head(operands):
        query_head, key_head, value_head, ctx_key_head, ctx_value_head, bias_table = operands
        query_f = query_head.astype(jnp.float32)
        key_win = key_head[row_index].astype(jnp.float32)
        val_win = value_head[row_index].astype(jnp.float32)
        bias_win = bias_table[row_off[:, None, :, None], col_off[None, :, None, :]]
        scores_win = jnp.einsum('rqd,rkwd->rqkw', query_f, key_win) * inv_scale + bias_win
        scores_win = jnp.where(col_in[None, :, None, :], scores_win, NEG_BIG)
        scores_ctx = jnp.einsum('rqd,cd->rqc', query_f, ctx_key_head.astype(jnp.float32)) * inv_scale
        row_max = jnp.maximum(lax.optimization_barrier(jnp.max(scores_win, axis=(2, 3))), lax.optimization_barrier(jnp.max(scores_ctx, axis=2)))
        exp_win = jnp.exp(scores_win - row_max[:, :, None, None])
        exp_ctx = jnp.exp(scores_ctx - row_max[:, :, None])
        row_total = lax.optimization_barrier(jnp.sum(exp_win, axis=(2, 3))) + lax.optimization_barrier(jnp.sum(exp_ctx, axis=2))
        probs_win = (exp_win / row_total[:, :, None, None]).astype(jnp.bfloat16)
        probs_ctx = (exp_ctx / row_total[:, :, None]).astype(jnp.bfloat16)
        mixed_head = jnp.einsum('rqkw,rkwd->rqd', probs_win.astype(jnp.float32), val_win)
        mixed_head = mixed_head + jnp.einsum('rqc,cd->rqd', probs_ctx.astype(jnp.float32), ctx_value_head.astype(jnp.float32))
        return mixed_head.astype(jnp.bfloat16)
    attended = lax.map(per_head, (grid_heads(queries), grid_heads(lat_keys), grid_heads(lat_values), ctx_heads(ctx_keys), ctx_heads(ctx_values), rel_bias))
    attended = jnp.transpose(attended, (1, 2, 0, 3)).reshape(-1, HEADS * HEAD_DIM)
    head_cols = HEADS // N_TP * HEAD_DIM
    branch = jnp.zeros(latent.shape, jnp.float32)
    for group_idx in range(N_TP):
        low = group_idx * head_cols
        part_sum = jnp.dot(attended[:, low:low + head_cols], w_out[low:low + head_cols], preferred_element_type=jnp.float32).astype(jnp.bfloat16)
        part_sum = lax.optimization_barrier(part_sum)
        branch = branch + part_sum.astype(jnp.float32)
    return (latent.astype(jnp.float32) + gate_vec * branch).astype(jnp.bfloat16)
```

```python
import functools

import jax
import jax.numpy as jnp
from jax import lax
from jax.experimental import pallas as pl
from jax.experimental.pallas import tpu as pltpu
from jax.sharding import PartitionSpec as P

HEAD_DIM = 128
GRID_W = 32
WIN_H = 8
WIN_W = 16
HALF = WIN_H // 2
NORM_EPS = 1e-06
NEG_BIG = -1e30
MESH = pl.DeviceIdType.MESH
VMEM = pltpu.VMEM


def gather_kernel(
    sp, tp, act_ref, wsh_ref, wsc_ref, wg_ref, lat_ref, ctx_ref,
    mod_out, lat_out, ctx_out,
    part, mod_buf,
    m_send, m_recv, mf_send, mf_recv, own_send, own_recv,
    h_send, h_recv, hf_send, hf_recv, c_send, c_recv, cf_send, cf_recv, loc_sem,
):
    s = lax.axis_index("sp")
    t = lax.axis_index("tp")
    rows = lat_ref.shape[0]
    crow = ctx_ref.shape[0]
    cw = ctx_ref.shape[1] // tp
    tokens = rows * tp
    halo = tokens // 2

    def remote(src, dst, ss, rs, dev):
        return pltpu.make_async_remote_copy(
            src_ref=src, dst_ref=dst, send_sem=ss, recv_sem=rs,
            device_id=dev, device_id_type=MESH,
        )

    def sp_peer(d):
        return lax.rem(s + d, sp)

    def tp_peer(d):
        return lax.rem(t + d, tp)

    barrier = pltpu.get_barrier_semaphore()

    def greet(d, c):
        pl.semaphore_signal(barrier, inc=1, device_id=(sp_peer(d), t), device_id_type=MESH)
        return c

    lax.fori_loop(1, sp, greet, 0)
    for d in range(1, tp):
        pl.semaphore_signal(barrier, inc=1, device_id=(s, tp_peer(d)), device_id_type=MESH)

    def act(k):
        return act_ref[8 * k : 8 * k + 8, :].astype(jnp.bfloat16)

    val = (
        jnp.dot(act(0), wsh_ref[...], preferred_element_type=jnp.float32)
        + jnp.dot(act(1), wsc_ref[...], preferred_element_type=jnp.float32)
        + jnp.dot(act(2), wg_ref[...], preferred_element_type=jnp.float32)
    )
    part[...] = val
    mod_buf[pl.ds(s, 1)] = val[None]

    pl.semaphore_wait(barrier, sp - 1 + tp - 1)

    def mod_copy(d, src):
        return remote(part, mod_buf.at[src], m_send.at[d], m_recv.at[d], (sp_peer(d), t))

    def send_mod(d, c):
        mod_copy(d, s).start()
        return c

    lax.fori_loop(1, sp, send_mod, 0)

    def own_rows(who):
        return lat_out.at[pl.ds(pl.multiple_of(halo + who * rows, rows), rows), :]

    for d in range(1, tp):
        remote(lat_ref, own_rows(t), own_send.at[d], own_recv.at[d], (s, tp_peer(d))).start()
    local_lat = pltpu.make_async_copy(lat_ref, own_rows(t), loc_sem.at[0])
    local_lat.start()
    local_ctx = pltpu.make_async_copy(
        ctx_ref, ctx_out.at[pl.ds(pl.multiple_of(s * crow, crow), crow), :], loc_sem.at[1]
    )
    local_ctx.start()

    upper = t >= tp // 2

    def halo_rows(who):
        off = jnp.where(
            who >= tp // 2, (who - tp // 2) * rows, halo + tokens + who * rows
        )
        return lat_out.at[pl.ds(pl.multiple_of(off, rows), rows), :]

    halo_dev = jnp.where(upper, lax.rem(s + 1, sp), lax.rem(s + sp - 1, sp))
    halo_copy = remote(lat_ref, halo_rows(t), h_send, h_recv, (halo_dev, t))
    halo_copy.start()

    def ctx_block(src, who):
        return ctx_out.at[
            pl.ds(pl.multiple_of(src * crow, crow), crow),
            pl.ds(pl.multiple_of(who * cw, cw), cw),
        ]

    def ctx_copy(d, src):
        return remote(
            ctx_ref.at[:, pl.ds(pl.multiple_of(t * cw, cw), cw)],
            ctx_block(src, t), c_send.at[d], c_recv.at[d], (sp_peer(d), t),
        )

    def send_ctx(d, c):
        ctx_copy(d, s).start()
        return c

    lax.fori_loop(1, sp, send_ctx, 0)

    def recv_mod(d, c):
        mod_copy(d, lax.rem(s + sp - d, sp)).wait_recv()
        return c

    lax.fori_loop(1, sp, recv_mod, 0)
    mod_out[pl.ds(t, 1)] = jnp.sum(mod_buf[...], axis=0, keepdims=True)

    def mod_fwd(d, who):
        return remote(
            mod_out.at[who], mod_out.at[who], mf_send.at[d], mf_recv.at[d], (s, tp_peer(d))
        )

    for d in range(1, tp):
        mod_fwd(d, t).start()

    def halo_fwd(d, who):
        return remote(
            halo_rows(who), halo_rows(who), hf_send.at[d], hf_recv.at[d], (s, tp_peer(d))
        )

    halo_copy.wait_recv()
    for d in range(1, tp):
        halo_fwd(d, t).start()

    def ctx_fwd(d, e, src, who):
        return remote(
            ctx_block(src, who), ctx_block(src, who),
            cf_send.at[d, e], cf_recv.at[d, e], (s, tp_peer(e)),
        )

    def relay_ctx(d, c):
        src = lax.rem(s + sp - d, sp)
        ctx_copy(d, src).wait_recv()
        for e in range(1, tp):
            ctx_fwd(d, e, src, t).start()
        return c

    lax.fori_loop(1, sp, relay_ctx, 0)

    for d in range(1, tp):
        who = lax.rem(t + tp - d, tp)
        remote(lat_ref, own_rows(who), own_send.at[d], own_recv.at[d], (s, tp_peer(d))).wait()
        mod_fwd(d, who).wait()
        halo_fwd(d, who).wait()

    def finish(d, c):
        src = lax.rem(s + sp - d, sp)
        for e in range(1, tp):
            ctx_fwd(d, e, src, lax.rem(t + tp - e, tp)).wait()
        mod_copy(d, s).wait_send()
        ctx_copy(d, s).wait_send()
        return c

    lax.fori_loop(1, sp, finish, 0)
    halo_copy.wait_send()
    local_lat.wait()
    local_ctx.wait()


def gather_all(sp, tp, acts, w_shift, w_scale, w_gate, latent, context):
    width = latent.shape[1]
    cols = w_shift.shape[1]
    tokens = latent.shape[0] * tp
    dma = pltpu.SemaphoreType.DMA
    spec = pl.BlockSpec(memory_space=VMEM)
    return pl.pallas_call(
        functools.partial(gather_kernel, sp, tp),
        out_shape=(
            jax.ShapeDtypeStruct((tp, 8, cols), jnp.float32),
            jax.ShapeDtypeStruct((2 * tokens, width), jnp.bfloat16),
            jax.ShapeDtypeStruct((context.shape[0] * sp, width), jnp.bfloat16),
        ),
        in_specs=[spec] * 6,
        out_specs=(spec,) * 3,
        scratch_shapes=[
            VMEM((8, cols), jnp.float32),
            VMEM((sp, 8, cols), jnp.float32),
            dma((sp,)), dma((sp,)), dma((tp,)), dma((tp,)), dma((tp,)), dma((tp,)),
            dma, dma, dma((tp,)), dma((tp,)), dma((sp,)), dma((sp,)),
            dma((sp, tp)), dma((sp, tp)), dma((2,)),
        ],
        compiler_params=pltpu.CompilerParams(collective_id=0, has_side_effects=True),
        name="gather_all",
    )(acts, w_shift, w_scale, w_gate, latent, context)


def attend_kernel(sp, tokens, n_lat, q_ref, k_ref, v_ref, tab_ref, o_ref):
    rows = tokens // GRID_W
    lanes = lax.broadcasted_iota(jnp.int32, (GRID_W, 128), 1)
    cq = lax.broadcasted_iota(jnp.int32, (GRID_W, 128), 0)
    c2 = lanes % GRID_W
    cs = jnp.clip(cq - WIN_W // 2, 0, GRID_W - WIN_W)
    col_in = (c2 >= cs) & (c2 < cs + WIN_W)
    per = 128 // GRID_W
    groups = []
    for k in range(24 // per):
        acc = jnp.full((GRID_W, 128), NEG_BIG, jnp.float32)
        for g in range(per):
            row = jnp.broadcast_to(tab_ref[0, per * k + g : per * k + g + 1, :], (GRID_W, 128))
            shift = (GRID_W * g - (WIN_W - 1)) % 128
            rolled = pltpu.roll(row, shift, 1, stride=1, stride_axis=0)
            acc = jnp.where(lanes // GRID_W == g, rolled, acc)
        groups.append(jnp.where(col_in, acc, NEG_BIG))
    table = jnp.concatenate(groups, axis=1)
    total = table.shape[1]
    first = lax.axis_index("sp") * rows
    all_rows = rows * sp
    kr = lax.broadcasted_iota(jnp.int32, (GRID_W, n_lat), 1) // GRID_W
    strips = []
    for r in range(rows):
        shift = (rows - 1 - r) * GRID_W
        strip = table if shift == 0 else pltpu.roll(table, total - shift, 1)
        lo = jnp.clip(first + r - HALF, 0, all_rows - WIN_H) - first + HALF
        strips.append(jnp.where((kr >= lo) & (kr < lo + WIN_H), strip[:, :n_lat], NEG_BIG))
    bias = jnp.concatenate(strips, axis=0)
    scores = lax.dot_general(
        q_ref[...], k_ref[...], (((1,), (1,)), ((), ())), preferred_element_type=jnp.float32
    ) * (HEAD_DIM ** -0.5)
    win = scores[:, :n_lat] + bias
    ctx = scores[:, n_lat:]
    top = jnp.maximum(
        jnp.max(win, axis=1, keepdims=True), jnp.max(ctx, axis=1, keepdims=True)
    )
    e_win = jnp.exp(win - top)
    e_ctx = jnp.exp(ctx - top)
    denom = jnp.sum(e_win, axis=1, keepdims=True) + jnp.sum(e_ctx, axis=1, keepdims=True)
    probs = jnp.concatenate([e_win.astype(jnp.bfloat16), e_ctx.astype(jnp.bfloat16)], axis=1)
    out = jnp.dot(probs, v_ref[...], preferred_element_type=jnp.float32)
    o_ref[...] = (out / denom).astype(jnp.bfloat16)


def attend(sp, n_lat, queries, keys, values, table):
    tokens, cols = queries.shape
    kv = keys.shape[0]
    heads = cols // HEAD_DIM
    return pl.pallas_call(
        functools.partial(attend_kernel, sp, tokens, n_lat),
        grid=(heads,),
        out_shape=jax.ShapeDtypeStruct((tokens, cols), jnp.bfloat16),
        in_specs=[
            pl.BlockSpec((tokens, HEAD_DIM), lambda h: (0, h)),
            pl.BlockSpec((kv, HEAD_DIM), lambda h: (0, h)),
            pl.BlockSpec((kv, HEAD_DIM), lambda h: (0, h)),
            pl.BlockSpec((1, 24, 128), lambda h: (h, 0, 0)),
        ],
        out_specs=pl.BlockSpec((tokens, HEAD_DIM), lambda h: (0, h)),
        name="attend",
    )(queries, keys, values, table)


def output_kernel(tp, att_ref, w_ref, lat_ref, gate_ref, out_ref, sbuf, rbuf, send, recv):
    s = lax.axis_index("sp")
    t = lax.axis_index("tp")
    rows = lat_ref.shape[0]
    n_chunk = sbuf.shape[1]
    cw = sbuf.shape[3]
    barrier = pltpu.get_barrier_semaphore()
    for d in range(1, tp):
        pl.semaphore_signal(
            barrier, inc=1, device_id=(s, lax.rem(t + d, tp)), device_id_type=MESH
        )

    def product(who, c):
        a = att_ref[pl.ds(pl.multiple_of(who * rows, rows), rows), :]
        w = w_ref[:, c * cw : (c + 1) * cw]
        return jnp.dot(a, w, preferred_element_type=jnp.float32).astype(jnp.bfloat16)

    def copy(d, c):
        return pltpu.make_async_remote_copy(
            src_ref=sbuf.at[d, c], dst_ref=rbuf.at[d, c],
            send_sem=send.at[d, c], recv_sem=recv.at[d, c],
            device_id=(s, lax.rem(t + d, tp)), device_id_type=MESH,
        )

    for d in range(1, tp):
        for c in range(n_chunk):
            sbuf[d, c] = product(lax.rem(t + d, tp), c)
            if d == 1 and c == 0:
                pl.semaphore_wait(barrier, tp - 1)
            copy(d, c).start()
    for c in range(n_chunk):
        branch = product(t, c).astype(jnp.float32)
        for d in range(1, tp):
            copy(d, c).wait_recv()
            branch = branch + rbuf[d, c].astype(jnp.float32)
        sl = slice(c * cw, (c + 1) * cw)
        out_ref[:, sl] = (
            lat_ref[:, sl].astype(jnp.float32) + gate_ref[:, sl] * branch
        ).astype(jnp.bfloat16)
    for d in range(1, tp):
        for c in range(n_chunk):
            copy(d, c).wait_send()


def output(tp, attended, w_out, latent, gate):
    rows, width = latent.shape
    n_chunk = 4
    cw = width // n_chunk
    spec = pl.BlockSpec(memory_space=VMEM)
    dma = pltpu.SemaphoreType.DMA
    return pl.pallas_call(
        functools.partial(output_kernel, tp),
        out_shape=jax.ShapeDtypeStruct(latent.shape, jnp.bfloat16),
        in_specs=[spec] * 4,
        out_specs=spec,
        scratch_shapes=[
            VMEM((tp, n_chunk, rows, cw), jnp.bfloat16),
            VMEM((tp, n_chunk, rows, cw), jnp.bfloat16),
            dma((tp, n_chunk)), dma((tp, n_chunk)),
        ],
        compiler_params=pltpu.CompilerParams(collective_id=1, has_side_effects=True),
        name="output",
    )(attended, w_out, latent, gate)


def rms_mod(block, norm_gain, shifts, scales):
    block = block.astype(jnp.float32)
    normed = (
        block * lax.rsqrt(jnp.mean(block * block, axis=-1, keepdims=True) + NORM_EPS) * norm_gain
    )
    return (normed * (1.0 + scales) + shifts).astype(jnp.bfloat16)


def on_device(
    latent, context, condition, ctx_cond, norm_gain, w_shift, w_scale, w_gate,
    w_query, w_key, w_value, w_out, rel_bias,
):
    tp = lax.axis_size("tp")
    sp = lax.axis_size("sp")
    head_dev = w_query.shape[1] // HEAD_DIM
    row_part = w_shift.shape[0]
    tokens = latent.shape[0] * tp
    halo = HALF * GRID_W
    assert tokens == 2 * halo and tp % 2 == 0
    pair = jnp.stack([condition, ctx_cond])
    pair = lax.dynamic_slice_in_dim(pair, lax.axis_index("sp") * row_part, row_part, 1)
    activated = jax.nn.silu(pair).astype(jnp.bfloat16).astype(jnp.float32)
    acts = jnp.concatenate(
        [
            jnp.pad(activated, ((0, 6), (0, 0))),
            jnp.pad(activated, ((2, 4), (0, 0))),
            jnp.pad(activated[:1], ((4, 3), (0, 0))),
        ]
    )
    mod, lat_all, ctx_all = gather_all(
        sp, tp, acts, w_shift, w_scale, w_gate, latent, context
    )
    mod = jnp.concatenate([mod[i] for i in range(tp)], axis=1)
    normed = jnp.concatenate(
        [
            rms_mod(lat_all, norm_gain, mod[0], mod[2]),
            rms_mod(ctx_all, norm_gain, mod[1], mod[3]),
        ]
    )

    def proj(x, w):
        return jnp.dot(x, w, preferred_element_type=jnp.float32).astype(jnp.bfloat16)

    queries = proj(normed[halo : halo + tokens], w_query)
    keys = proj(normed, w_key)
    values = proj(normed, w_value)
    table = lax.dynamic_slice_in_dim(rel_bias, lax.axis_index("tp") * head_dev, head_dev, 0)
    table = jnp.pad(
        table, ((0, 0), (HALF, 24 - HALF - table.shape[1]), (0, 128 - table.shape[2]))
    )
    attended = attend(sp, 2 * tokens, queries, keys, values, table)
    return output(tp, attended, w_out, latent, mod[4:5])


def solution(mesh):
    placed = (
        P(("sp", "tp"), None),
        P("sp", None),
        P(),
        P(),
        P(),
        P("sp", "tp"),
        P("sp", "tp"),
        P("sp", "tp"),
        P(None, "tp"),
        P(None, "tp"),
        P(None, "tp"),
        P("tp", None),
        P(),
    )
    return jax.shard_map(
        on_device, mesh=mesh, in_specs=placed, out_specs=P(("sp", "tp"), None), check_vma=False
    )
```

```python
import functools

import jax
import jax.numpy as jnp
from jax import lax
from jax.experimental import pallas as pl
from jax.experimental.pallas import tpu as pltpu
from jax.sharding import PartitionSpec as P

HEAD_DIM = 128
GRID_W = 32
WIN_H = 8
WIN_W = 16
HALF = WIN_H // 2
INNER = 4
NORM_EPS = 1e-06
NEG_BIG = -1e30
MESH = pl.DeviceIdType.MESH
VMEM = pltpu.VMEM


def gather_kernel(
    sp, tp, act_ref, wsh_ref, wsc_ref, wg_ref, lat_ref, ctx_ref,
    mod_out, lat_out, ctx_out,
    in_buf, out_buf, mi_send, mi_recv, mo_send, mo_recv, mf_send, mf_recv,
    own_send, own_recv, h_send, h_recv, hf_send, hf_recv,
    z_send, z_recv, n_send, n_recv, d_send, d_recv, f_send, f_recv, loc_sem,
):
    s = lax.axis_index("sp")
    t = lax.axis_index("tp")
    n_o = sp // INNER
    o = s // INNER
    i = lax.rem(s, INNER)
    rows = lat_ref.shape[0]
    crow = ctx_ref.shape[0]
    cw = ctx_ref.shape[1] // tp
    hw = cw // 2
    tokens = rows * tp
    halo = tokens // 2

    def remote(src, dst, ss, rs, dev):
        return pltpu.make_async_remote_copy(
            src_ref=src, dst_ref=dst, send_sem=ss, recv_sem=rs,
            device_id=dev, device_id_type=MESH,
        )

    def at(oo, ii):
        return (oo * INNER + ii, t)

    def outer(d):
        return lax.rem(o + d, n_o)

    def inner(d):
        return lax.rem(i + d, INNER)

    def tp_peer(d):
        return lax.rem(t + d, tp)

    ix = i + 1 - 2 * lax.rem(i, 2)
    iy = lax.rem(i + 2, INNER)
    ixy = lax.rem(ix + 2, INNER)
    nbr = (ix, iy)
    nxt = (lax.rem(s + 1, sp), t)
    prv = (lax.rem(s + sp - 1, sp), t)

    barrier = pltpu.get_barrier_semaphore()

    def greet(dev):
        pl.semaphore_signal(barrier, inc=1, device_id=dev, device_id_type=MESH)

    for d in range(1, n_o):
        greet(at(outer(d), i))
    for d in range(1, INNER):
        greet(at(o, inner(d)))
    for d in range(1, tp):
        greet((s, tp_peer(d)))
    greet(nxt)
    greet(prv)

    def act(k):
        return act_ref[8 * k : 8 * k + 8, :].astype(jnp.bfloat16)

    val = (
        jnp.dot(act(0), wsh_ref[...], preferred_element_type=jnp.float32)
        + jnp.dot(act(1), wsc_ref[...], preferred_element_type=jnp.float32)
        + jnp.dot(act(2), wg_ref[...], preferred_element_type=jnp.float32)
    )
    in_buf[pl.ds(i, 1)] = val[None]

    pl.semaphore_wait(barrier, n_o - 1 + INNER - 1 + tp - 1 + 2)

    def mod_in(d, who):
        return remote(
            in_buf.at[who], in_buf.at[who], mi_send.at[d], mi_recv.at[d], at(o, inner(d))
        )

    def mod_across(d, who):
        return remote(
            out_buf.at[who], out_buf.at[who], mo_send.at[d], mo_recv.at[d], at(outer(d), i)
        )

    def mod_fwd(d, who):
        return remote(
            mod_out.at[who], mod_out.at[who], mf_send.at[d], mf_recv.at[d], (s, tp_peer(d))
        )

    for d in range(1, INNER):
        mod_in(d, i).start()

    def own_rows(who):
        return lat_out.at[pl.ds(pl.multiple_of(halo + who * rows, rows), rows), :]

    def own_copy(d, who):
        return remote(lat_ref, own_rows(who), own_send.at[d], own_recv.at[d], (s, tp_peer(d)))

    def halo_rows(who):
        off = jnp.where(
            who >= tp // 2, (who - tp // 2) * rows, halo + tokens + who * rows
        )
        return lat_out.at[pl.ds(pl.multiple_of(off, rows), rows), :]

    halo_dev = (jnp.where(t >= tp // 2, nxt[0], prv[0]), t)
    halo_copy = remote(lat_ref, halo_rows(t), h_send, h_recv, halo_dev)

    def halo_fwd(d, who):
        return remote(
            halo_rows(who), halo_rows(who), hf_send.at[d], hf_recv.at[d], (s, tp_peer(d))
        )

    def block(oo, ii, who, half=None):
        off = who * cw + (0 if half is None else half * hw)
        size = cw if half is None else hw
        return ctx_out.at[
            pl.ds(pl.multiple_of((oo * INNER + ii) * crow, crow), crow),
            pl.ds(pl.multiple_of(off, hw), size),
        ]

    mine = ctx_ref.at[:, pl.ds(pl.multiple_of(t * cw, cw), cw)]

    def line(d, oo):
        return remote(mine, block(oo, i, t), z_send.at[d], z_recv.at[d], at(outer(d), i))

    def held(j):
        return lax.rem(o + n_o - j, n_o)

    def side(j, a, ii):
        src = mine if j == 0 else block(held(j), ii, t)
        return remote(
            src, block(held(j), ii, t), n_send.at[j, a], n_recv.at[j, a], at(o, nbr[a])
        )

    def diag(j, a, ii):
        ref = block(held(j), ii, t, a)
        return remote(ref, ref, d_send.at[j, a], d_recv.at[j, a], at(o, nbr[1 - a]))

    def share(e, j, k, who):
        half = None if k < 3 else k - 3
        ref = block(held(j), (i, ix, iy, ixy, ixy)[k], who, half)
        return remote(
            ref, ref, f_send.at[e, j, k], f_recv.at[e, j, k], (s, tp_peer(e))
        )

    def share_all(j, k):
        for e in range(1, tp):
            share(e, j, k, t).start()

    for d in range(1, n_o):
        line(d, o).start()
    for a in range(2):
        side(0, a, i).start()
    for d in range(1, tp):
        own_copy(d, t).start()
    local_lat = pltpu.make_async_copy(lat_ref, own_rows(t), loc_sem.at[0])
    local_lat.start()
    local_ctx = pltpu.make_async_copy(
        ctx_ref, ctx_out.at[pl.ds(pl.multiple_of(s * crow, crow), crow), :], loc_sem.at[1]
    )
    local_ctx.start()

    for d in range(1, INNER):
        mod_in(d, lax.rem(i + INNER - d, INNER)).wait_recv()
    out_buf[pl.ds(o, 1)] = jnp.sum(in_buf[...], axis=0, keepdims=True)
    for d in range(1, n_o):
        mod_across(d, o).start()
    halo_copy.start()
    for d in range(1, n_o):
        mod_across(d, held(d)).wait_recv()
    mod_out[pl.ds(t, 1)] = jnp.sum(out_buf[...], axis=0, keepdims=True)
    for d in range(1, tp):
        mod_fwd(d, t).start()

    def relay(j):
        for a in range(2):
            side(j, a, nbr[a]).wait_recv()
            diag(j, a, nbr[a]).start()
            share_all(j, 1 + a)

    for j in range(1, n_o):
        line(j, held(j)).wait_recv()
        for a in range(2):
            side(j, a, i).start()
        share_all(j, 0)
        relay(j - 1)
        if j == 1:
            halo_copy.wait_recv()
            for d in range(1, tp):
                halo_fwd(d, t).start()
    relay(n_o - 1)
    for j in range(n_o):
        for a in range(2):
            diag(j, a, ixy).wait_recv()
            share_all(j, 3 + a)

    for d in range(1, tp):
        who = lax.rem(t + tp - d, tp)
        own_copy(d, who).wait()
        mod_fwd(d, who).wait()
        halo_fwd(d, who).wait()
    for j in range(n_o):
        for k in range(5):
            if j == 0 and k == 0:
                continue
            for e in range(1, tp):
                share(e, j, k, lax.rem(t + tp - e, tp)).wait()
        for a in range(2):
            side(j, a, i).wait_send()
            diag(j, a, nbr[a]).wait_send()
    for d in range(1, n_o):
        line(d, o).wait_send()
        mod_across(d, o).wait_send()
    for d in range(1, INNER):
        mod_in(d, i).wait_send()
    halo_copy.wait_send()
    local_lat.wait()
    local_ctx.wait()


def gather_all(sp, tp, acts, w_shift, w_scale, w_gate, latent, context):
    width = latent.shape[1]
    cols = w_shift.shape[1]
    tokens = latent.shape[0] * tp
    n_o = sp // INNER
    dma = pltpu.SemaphoreType.DMA
    spec = pl.BlockSpec(memory_space=VMEM)
    return pl.pallas_call(
        functools.partial(gather_kernel, sp, tp),
        out_shape=(
            jax.ShapeDtypeStruct((tp, 8, cols), jnp.float32),
            jax.ShapeDtypeStruct((2 * tokens, width), jnp.bfloat16),
            jax.ShapeDtypeStruct((context.shape[0] * sp, width), jnp.bfloat16),
        ),
        in_specs=[spec] * 6,
        out_specs=(spec,) * 3,
        scratch_shapes=[
            VMEM((INNER, 8, cols), jnp.float32),
            VMEM((n_o, 8, cols), jnp.float32),
            dma((INNER,)), dma((INNER,)), dma((n_o,)), dma((n_o,)), dma((tp,)), dma((tp,)),
            dma((tp,)), dma((tp,)), dma, dma, dma((tp,)), dma((tp,)),
            dma((n_o,)), dma((n_o,)), dma((n_o, 2)), dma((n_o, 2)),
            dma((n_o, 2)), dma((n_o, 2)), dma((tp, n_o, 5)), dma((tp, n_o, 5)), dma((2,)),
        ],
        compiler_params=pltpu.CompilerParams(collective_id=0, has_side_effects=True),
        name="gather_all",
    )(acts, w_shift, w_scale, w_gate, latent, context)


def attend_kernel(sp, tokens, n_lat, q_ref, k_ref, v_ref, tab_ref, o_ref):
    rows = tokens // GRID_W
    lanes = lax.broadcasted_iota(jnp.int32, (GRID_W, 128), 1)
    cq = lax.broadcasted_iota(jnp.int32, (GRID_W, 128), 0)
    c2 = lanes % GRID_W
    cs = jnp.clip(cq - WIN_W // 2, 0, GRID_W - WIN_W)
    col_in = (c2 >= cs) & (c2 < cs + WIN_W)
    per = 128 // GRID_W
    groups = []
    for k in range(24 // per):
        acc = jnp.full((GRID_W, 128), NEG_BIG, jnp.float32)
        for g in range(per):
            row = jnp.broadcast_to(tab_ref[0, per * k + g : per * k + g + 1, :], (GRID_W, 128))
            shift = (GRID_W * g - (WIN_W - 1)) % 128
            rolled = pltpu.roll(row, shift, 1, stride=1, stride_axis=0)
            acc = jnp.where(lanes // GRID_W == g, rolled, acc)
        groups.append(jnp.where(col_in, acc, NEG_BIG))
    table = jnp.concatenate(groups, axis=1)
    total = table.shape[1]
    first = lax.axis_index("sp") * rows
    all_rows = rows * sp
    kr = lax.broadcasted_iota(jnp.int32, (GRID_W, n_lat), 1) // GRID_W
    strips = []
    for r in range(rows):
        shift = (rows - 1 - r) * GRID_W
        strip = table if shift == 0 else pltpu.roll(table, total - shift, 1)
        lo = jnp.clip(first + r - HALF, 0, all_rows - WIN_H) - first + HALF
        strips.append(jnp.where((kr >= lo) & (kr < lo + WIN_H), strip[:, :n_lat], NEG_BIG))
    bias = jnp.concatenate(strips, axis=0)
    scores = lax.dot_general(
        q_ref[...], k_ref[...], (((1,), (1,)), ((), ())), preferred_element_type=jnp.float32
    ) * (HEAD_DIM ** -0.5)
    win = scores[:, :n_lat] + bias
    ctx = scores[:, n_lat:]
    top = jnp.maximum(
        jnp.max(win, axis=1, keepdims=True), jnp.max(ctx, axis=1, keepdims=True)
    )
    e_win = jnp.exp(win - top)
    e_ctx = jnp.exp(ctx - top)
    denom = jnp.sum(e_win, axis=1, keepdims=True) + jnp.sum(e_ctx, axis=1, keepdims=True)
    probs = jnp.concatenate([e_win.astype(jnp.bfloat16), e_ctx.astype(jnp.bfloat16)], axis=1)
    out = jnp.dot(probs, v_ref[...], preferred_element_type=jnp.float32)
    o_ref[...] = (out / denom).astype(jnp.bfloat16)


def attend(sp, n_lat, queries, keys, values, table):
    tokens, cols = queries.shape
    kv = keys.shape[0]
    heads = cols // HEAD_DIM
    return pl.pallas_call(
        functools.partial(attend_kernel, sp, tokens, n_lat),
        grid=(heads,),
        out_shape=jax.ShapeDtypeStruct((tokens, cols), jnp.bfloat16),
        in_specs=[
            pl.BlockSpec((tokens, HEAD_DIM), lambda h: (0, h)),
            pl.BlockSpec((kv, HEAD_DIM), lambda h: (0, h)),
            pl.BlockSpec((kv, HEAD_DIM), lambda h: (0, h)),
            pl.BlockSpec((1, 24, 128), lambda h: (h, 0, 0)),
        ],
        out_specs=pl.BlockSpec((tokens, HEAD_DIM), lambda h: (0, h)),
        name="attend",
    )(queries, keys, values, table)


def output_kernel(tp, att_ref, w_ref, lat_ref, gate_ref, out_ref, sbuf, rbuf, send, recv):
    s = lax.axis_index("sp")
    t = lax.axis_index("tp")
    rows = lat_ref.shape[0]
    n_chunk = sbuf.shape[1]
    cw = sbuf.shape[3]
    barrier = pltpu.get_barrier_semaphore()
    for d in range(1, tp):
        pl.semaphore_signal(
            barrier, inc=1, device_id=(s, lax.rem(t + d, tp)), device_id_type=MESH
        )

    def product(who, c):
        a = att_ref[pl.ds(pl.multiple_of(who * rows, rows), rows), :]
        w = w_ref[:, c * cw : (c + 1) * cw]
        return jnp.dot(a, w, preferred_element_type=jnp.float32).astype(jnp.bfloat16)

    def copy(d, c):
        return pltpu.make_async_remote_copy(
            src_ref=sbuf.at[d, c], dst_ref=rbuf.at[d, c],
            send_sem=send.at[d, c], recv_sem=recv.at[d, c],
            device_id=(s, lax.rem(t + d, tp)), device_id_type=MESH,
        )

    for d in range(1, tp):
        for c in range(n_chunk):
            sbuf[d, c] = product(lax.rem(t + d, tp), c)
            if d == 1 and c == 0:
                pl.semaphore_wait(barrier, tp - 1)
            copy(d, c).start()
    for c in range(n_chunk):
        branch = product(t, c).astype(jnp.float32)
        for d in range(1, tp):
            copy(d, c).wait_recv()
            branch = branch + rbuf[d, c].astype(jnp.float32)
        sl = slice(c * cw, (c + 1) * cw)
        out_ref[:, sl] = (
            lat_ref[:, sl].astype(jnp.float32) + gate_ref[:, sl] * branch
        ).astype(jnp.bfloat16)
    for d in range(1, tp):
        for c in range(n_chunk):
            copy(d, c).wait_send()


def output(tp, attended, w_out, latent, gate):
    rows, width = latent.shape
    n_chunk = 4
    cw = width // n_chunk
    spec = pl.BlockSpec(memory_space=VMEM)
    dma = pltpu.SemaphoreType.DMA
    return pl.pallas_call(
        functools.partial(output_kernel, tp),
        out_shape=jax.ShapeDtypeStruct(latent.shape, jnp.bfloat16),
        in_specs=[spec] * 4,
        out_specs=spec,
        scratch_shapes=[
            VMEM((tp, n_chunk, rows, cw), jnp.bfloat16),
            VMEM((tp, n_chunk, rows, cw), jnp.bfloat16),
            dma((tp, n_chunk)), dma((tp, n_chunk)),
        ],
        compiler_params=pltpu.CompilerParams(collective_id=1, has_side_effects=True),
        name="output",
    )(attended, w_out, latent, gate)


def rms_mod(block, norm_gain, shifts, scales):
    block = block.astype(jnp.float32)
    normed = (
        block * lax.rsqrt(jnp.mean(block * block, axis=-1, keepdims=True) + NORM_EPS) * norm_gain
    )
    return (normed * (1.0 + scales) + shifts).astype(jnp.bfloat16)


def on_device(
    latent, context, condition, ctx_cond, norm_gain, w_shift, w_scale, w_gate,
    w_query, w_key, w_value, w_out, rel_bias,
):
    tp = lax.axis_size("tp")
    sp = lax.axis_size("sp")
    head_dev = w_query.shape[1] // HEAD_DIM
    row_part = w_shift.shape[0]
    tokens = latent.shape[0] * tp
    halo = HALF * GRID_W
    assert tokens == 2 * halo and tp % 2 == 0 and sp % INNER == 0
    pair = jnp.stack([condition, ctx_cond])
    pair = lax.dynamic_slice_in_dim(pair, lax.axis_index("sp") * row_part, row_part, 1)
    activated = jax.nn.silu(pair).astype(jnp.bfloat16).astype(jnp.float32)
    acts = jnp.concatenate(
        [
            jnp.pad(activated, ((0, 6), (0, 0))),
            jnp.pad(activated, ((2, 4), (0, 0))),
            jnp.pad(activated[:1], ((4, 3), (0, 0))),
        ]
    )
    mod, lat_all, ctx_all = gather_all(
        sp, tp, acts, w_shift, w_scale, w_gate, latent, context
    )
    mod = jnp.concatenate([mod[i] for i in range(tp)], axis=1)
    normed = jnp.concatenate(
        [
            rms_mod(lat_all, norm_gain, mod[0], mod[2]),
            rms_mod(ctx_all, norm_gain, mod[1], mod[3]),
        ]
    )

    def proj(x, w):
        return jnp.dot(x, w, preferred_element_type=jnp.float32).astype(jnp.bfloat16)

    queries = proj(normed[halo : halo + tokens], w_query)
    keys = proj(normed, w_key)
    values = proj(normed, w_value)
    table = lax.dynamic_slice_in_dim(rel_bias, lax.axis_index("tp") * head_dev, head_dev, 0)
    table = jnp.pad(
        table, ((0, 0), (HALF, 24 - HALF - table.shape[1]), (0, 128 - table.shape[2]))
    )
    attended = attend(sp, 2 * tokens, queries, keys, values, table)
    return output(tp, attended, w_out, latent, mod[4:5])


def solution(mesh):
    placed = (
        P(("sp", "tp"), None),
        P("sp", None),
        P(),
        P(),
        P(),
        P("sp", "tp"),
        P("sp", "tp"),
        P("sp", "tp"),
        P(None, "tp"),
        P(None, "tp"),
        P(None, "tp"),
        P("tp", None),
        P(),
    )
    return jax.shard_map(
        on_device, mesh=mesh, in_specs=placed, out_specs=P(("sp", "tp"), None), check_vma=False
    )
```
